128 devices in a mesh: rep: 2 (over z_hi), fs: 32 (over z_lo, y, x), tp: 2 (over core).
Axes of the slice: x: 4, y: 4, z: 4 (z_hi: 2, z_lo: 2; z = z_hi * 2 + z_lo), core: 2. Of those that a mesh axis runs over, the one named last changes fastest.
Arguments:
- sequence: bfloat16 [64, 768, 2048], P(('rep', 'fs'), None, 'tp'), may hold values from -6 to 6
- mix_gain: float32 [2048], replicated, may hold values from 0.1 to 1.9
- ffn_gain: float32 [2048], replicated, may hold values from 0.1 to 1.9
- proj_outer: float32 [2048, 2048], P(None, ('tp', 'fs')), may hold values from -0.125 to 0.125
- proj_inner: float32 [2048, 2048], P(None, ('tp', 'fs')), may hold values from -0.125 to 0.125
- proj_value: float32 [2048, 2048], P(None, ('tp', 'fs')), may hold values from -0.125 to 0.125
- proj_scales: float32 [3, 2048], P(None, 'tp'), may hold values from 0.5 to 2
- taps: float32 [3, 2048], P(None, 'tp'), may hold values from -3 to 3
- mix_out: float32 [2048, 2048], P('tp', 'fs'), may hold values from -0.125 to 0.125
- mix_out_scale: float32 [2048], P('fs'), may hold values from 0.5 to 2
- ffn_gate: float32 [2048, 2816], P(None, ('tp', 'fs')), may hold values from -0.125 to 0.125
- ffn_up: float32 [2048, 2816], P(None, ('tp', 'fs')), may hold values from -0.125 to 0.125
- ffn_scales: float32 [2, 2816], P(None, 'tp'), may hold values from 0.5 to 2
- ffn_down: float32 [2816, 2048], P('tp', 'fs'), may hold values from -0.109375 to 0.109375
- down_scale: float32 [2048], P('fs'), may hold values from 0.5 to 2
Outputs:
- layer_out: bfloat16 [64, 768, 2048], P(('rep', 'fs'), None, 'tp')
The draws below stay inside these ranges and needn't reach their ends.
All inputs are finite; a program needn't handle non-finite values.
Results may differ from the reference program's by a relative error of at most 0.013.
Values may be sent and summed in bfloat16 or wider, within the bound.
A program may use at most 128 MiB of HBM per device.

```python
import math
import jax
import jax.numpy as jnp
from jax import lax

D = 2048
FF = 2816
LENGTH = 768
SEQS = 64
N_TP = 2


def steps_of(own_key, extent, split, low, largest):
    level = 1.0
    for position, blocks in split:
        draws = jax.random.uniform(jax.random.fold_in(jax.random.fold_in(own_key, 6), position), (blocks,), jnp.float32, low / len(split), largest / len(split))
        level = level * jnp.repeat(jnp.exp(draws), extent[position] // blocks).reshape((-1,) + (1,) * (len(extent) - 1 - position))
    return level


def bell_draw(own_key, extent, scale, bound, shards=(), held_as=jnp.bfloat16):
    result = scale * jax.random.normal(own_key, extent, jnp.float32)
    if shards:
        result = result * steps_of(own_key, extent, shards, -0.22, 0.18)
    return jnp.clip(result, -bound, bound).astype(held_as)


def setup_inputs(seed: int = 0) -> dict:
    keys = jax.random.split(jax.random.key(seed), 16)
    return {
        "sequence": bell_draw(keys[0], (SEQS, LENGTH, D), 1.0, 6.0, ((0, 64), (2, 2))),
        "mix_gain": jnp.clip(1.0 + 0.18 * jax.random.normal(keys[1], (D,), jnp.float32), 0.1, 1.9),
        "ffn_gain": jnp.clip(1.0 + 0.18 * jax.random.normal(keys[2], (D,), jnp.float32), 0.1, 1.9),
        "proj_outer": bell_draw(keys[3], (D, D), D ** -0.5, 0.125, ((1, 64),), jnp.float32),
        "proj_inner": bell_draw(keys[4], (D, D), D ** -0.5, 0.125, ((1, 64),), jnp.float32),
        "proj_value": bell_draw(keys[5], (D, D), D ** -0.5, 0.125, ((1, 64),), jnp.float32),
        "proj_scales": jnp.clip(jnp.exp(math.log(2.0) - 1.3862944 * jax.random.uniform(keys[6], (3, D), jnp.float32) ** steps_of(keys[6], (3, D), ((1, 2),), -0.2, 0.2)), 0.5, 2.0),
        "taps": bell_draw(keys[7], (3, D), 0.6, 3.0, ((1, 2),), jnp.float32),
        "mix_out": bell_draw(keys[8], (D, D), D ** -0.5, 0.125, ((0, 2), (1, 32)), jnp.float32),
        "mix_out_scale": jnp.clip(jnp.exp(math.log(2.0) - 1.3862944 * jax.random.uniform(keys[9], (D,), jnp.float32) ** steps_of(keys[9], (D,), ((0, 32),), -0.2, 0.2)), 0.5, 2.0),
        "ffn_gate": bell_draw(keys[10], (D, FF), D ** -0.5, 0.125, ((1, 64),), jnp.float32),
        "ffn_up": bell_draw(keys[11], (D, FF), D ** -0.5, 0.125, ((1, 64),), jnp.float32),
        "ffn_scales": jnp.clip(jnp.exp(math.log(2.0) - 1.3862944 * jax.random.uniform(keys[12], (2, FF), jnp.float32) ** steps_of(keys[12], (2, FF), ((1, 2),), -0.2, 0.2)), 0.5, 2.0),
        "ffn_down": bell_draw(keys[13], (FF, D), FF ** -0.5, 0.109375, ((0, 2), (1, 32)), jnp.float32),
        "down_scale": jnp.clip(jnp.exp(math.log(2.0) - 1.3862944 * jax.random.uniform(keys[14], (D,), jnp.float32) ** steps_of(keys[14], (D,), ((0, 32),), -0.2, 0.2)), 0.5, 2.0),
    }


eps = 1e-06

def rms_rows(rows, gain):
    values = rows.astype(jnp.float32)
    scaled = values * lax.rsqrt(lax.optimization_barrier(jnp.mean(values * values, axis=-1, keepdims=True)) + eps)
    return (scaled * gain).astype(jnp.bfloat16)

def split_sum(inputs, weight, scale):
    block = inputs.shape[1] // N_TP
    total = jnp.zeros((inputs.shape[0], weight.shape[1]), jnp.float32)
    for index in range(N_TP):
        part = jnp.dot(inputs[:, index * block:(index + 1) * block], weight[index * block:(index + 1) * block], preferred_element_type=jnp.float32) * scale
        rounded = lax.optimization_barrier(part.astype(jnp.bfloat16))
        total = total + rounded.astype(jnp.float32)
    return total

def reference(sequence, mix_gain, ffn_gain, proj_outer, proj_inner, proj_value, proj_scales, taps, mix_out, mix_out_scale, ffn_gate, ffn_up, ffn_scales, ffn_down, down_scale):
    w_outer = proj_outer.astype(jnp.bfloat16)
    w_inner = proj_inner.astype(jnp.bfloat16)
    w_value = proj_value.astype(jnp.bfloat16)
    w_mixout = mix_out.astype(jnp.bfloat16)
    w_gate = ffn_gate.astype(jnp.bfloat16)
    w_up = ffn_up.astype(jnp.bfloat16)
    w_down = ffn_down.astype(jnp.bfloat16)

    def layer(rows):
        normed = rms_rows(rows, mix_gain)
        outer = jnp.dot(normed, w_outer, preferred_element_type=jnp.float32) * proj_scales[0]
        inner = jnp.dot(normed, w_inner, preferred_element_type=jnp.float32) * proj_scales[1]
        value = jnp.dot(normed, w_value, preferred_element_type=jnp.float32) * proj_scales[2]
        carried = inner * value
        length = carried.shape[0]
        back_one = jnp.pad(carried, ((1, 0), (0, 0)))[:length]
        back_two = jnp.pad(carried, ((2, 0), (0, 0)))[:length]
        conv = taps[0] * back_two + taps[1] * back_one + taps[2] * carried
        gated = (outer * conv).astype(jnp.bfloat16)
        mix = split_sum(gated, w_mixout, mix_out_scale)
        after = (rows.astype(jnp.float32) + mix).astype(jnp.bfloat16)
        normed2 = rms_rows(after, ffn_gain)
        gate = jnp.dot(normed2, w_gate, preferred_element_type=jnp.float32) * ffn_scales[0]
        up = jnp.dot(normed2, w_up, preferred_element_type=jnp.float32) * ffn_scales[1]
        hidden = (jax.nn.silu(gate) * up).astype(jnp.bfloat16)
        ffn = split_sum(hidden, w_down, down_scale)
        return (after.astype(jnp.float32) + ffn).astype(jnp.bfloat16)
    return lax.map(layer, sequence)
```

```python
import functools

import jax
import jax.numpy as jnp
from jax import lax
from jax.experimental import pallas as pl
from jax.experimental.pallas import tpu as pltpu
from jax.sharding import PartitionSpec as P

F32, BF16 = jnp.float32, jnp.bfloat16
MESH = pl.DeviceIdType.MESH
EPS = 1e-06
D, L, HALF, FFB = 2048, 768, 1024, 48
HALO = 16
UP = L // 2 + HALO
LOW = L // 2
FR = UP + LOW
N_COPIES = 160


def dot_t(a, b):
    return lax.dot_general(a, b, (((1,), (1,)), ((), ())), preferred_element_type=F32)


def kernel(
    seq, wp, wm, wg, wd, taps, out,
    p_all, m_all, g_all, d_all, xo, xf, go, gf, c_s, rs_o, rs_f,
    snd_o, snd_f, rcv_o, rcv_f, keep, fsum, rcv_z, af, hid, fsnd, frcv, res,
    send_sem, recv_sem, loc_sem,
):
    rep, fs, tp = lax.axis_index("rep"), lax.axis_index("fs"), lax.axis_index("tp")
    zl, y, x = fs // 16, (fs // 4) % 4, fs % 4
    z = rep * 2 + zl
    xl, xr, yl, yr = (x + 3) % 4, (x + 1) % 4, (y + 3) % 4, (y + 1) % 4
    xa, ya = (x + 2) % 4, (y + 2) % 4
    zo = 1 - zl

    def plane(yy, xx):
        return {"fs": zl * 16 + yy * 4 + xx}

    def vert(zz):
        return {"rep": zz // 2, "fs": (zz % 2) * 16 + y * 4 + x}

    to_xl, to_xr, to_yl, to_yr = plane(y, xl), plane(y, xr), plane(yl, x), plane(yr, x)
    to_zl, to_zr = vert((z + 3) % 4), vert((z + 1) % 4)
    to_tp = {"tp": 1 - tp}

    count = [0]
    sent = []

    def send(src, dst, dev):
        k = count[0]
        count[0] += 1
        copy = pltpu.make_async_remote_copy(
            src_ref=src, dst_ref=dst, send_sem=send_sem.at[k], recv_sem=recv_sem.at[k],
            device_id=dev, device_id_type=MESH,
        )
        copy.start()
        sent.append(copy)
        return copy

    my_cols = pl.ds(pl.multiple_of(tp * HALF, HALF), HALF)

    local = [
        pltpu.make_async_copy(seq, xo.at[:, my_cols], loc_sem.at[0]),
        pltpu.make_async_copy(wg.at[0], g_all.at[0, zl, y, x], loc_sem.at[1]),
        pltpu.make_async_copy(wp, p_all.at[:, y, x], loc_sem.at[2]),
        pltpu.make_async_copy(wm.at[zl], m_all.at[zl, y, x], loc_sem.at[3]),
        pltpu.make_async_copy(wg.at[1], g_all.at[1, zl, y, x], loc_sem.at[4]),
        pltpu.make_async_copy(wd, d_all.at[zl, y, x], loc_sem.at[5]),
    ]
    for copy in local:
        copy.start()

    barrier = pltpu.get_barrier_semaphore()
    for dev in (to_xl, to_xr, to_yl, to_yr, to_zl, to_zr, to_tp):
        pl.semaphore_signal(barrier, inc=1, device_id=dev, device_id_type=MESH)
    pl.semaphore_wait(barrier, 7)

    class Gather:
        def __init__(self, block, depth):
            self.block, self.q = block, depth // 4
            self.c = {}

        def cols(self, stream, quarter=None):
            start = stream * 2 * self.q
            if quarter is None:
                return pl.ds(start, 2 * self.q)
            return pl.ds(start + quarter * self.q, self.q)

        def pair(self, name, u0, dev0, u1, dev1):
            self.c[name] = (send(u0, u0, dev0), send(u1, u1, dev1))

        def a1(self):
            b = self.block
            u = b(y, x, self.cols(0))
            self.pair("x1", u, to_xr, u, to_xl)
            u = b(y, x, self.cols(1))
            self.pair("y1", u, to_yr, u, to_yl)

        def got(self, name):
            for copy in self.c[name]:
                copy.wait_recv()

        def a2(self):
            b = self.block
            self.got("x1")
            self.pair("x2", b(y, xl, self.cols(0, 0)), to_xr, b(y, xr, self.cols(0, 1)), to_xl)
            self.got("y1")
            self.pair("y2", b(yl, x, self.cols(1, 0)), to_yr, b(yr, x, self.cols(1, 1)), to_yl)

        def a3(self):
            b, every = self.block, slice(None)
            self.got("x2")
            u = b(y, every, self.cols(0))
            self.pair("x3", u, to_yr, u, to_yl)
            self.got("y2")
            u = b(every, x, self.cols(1))
            self.pair("y3", u, to_xr, u, to_xl)

        def a4(self):
            b, every = self.block, slice(None)
            self.got("x3")
            self.pair("x4", b(yl, every, self.cols(0, 0)), to_yr, b(yr, every, self.cols(0, 1)), to_yl)
            self.got("y3")
            self.pair("y4", b(every, xl, self.cols(1, 0)), to_xr, b(every, xr, self.cols(1, 1)), to_xl)

        def a5(self):
            self.got("x4")
            self.got("y4")

        def z_units(self, names):
            b, every = self.block, slice(None)
            for yy, xx in names:
                u = b(yy, every, self.cols(0))
                w = b(every, xx, self.cols(1))
                self.pair(("z", len(self.c)), u, to_zr, w, to_zl)

        def z_own(self):
            self.z_units([(y, x)])

        def z_sides(self):
            self.z_units([(yl, xl), (yr, xr)])

        def z_far(self):
            self.z_units([(ya, xa)])

        def z_got(self):
            for name in list(self.c):
                if name[0] == "z":
                    self.got(name)

    gate = Gather(lambda yy, xx, k: g_all.at[0, zl, yy, xx, :, k], D)
    up = Gather(lambda yy, xx, k: g_all.at[1, zl, yy, xx, :, k], D)
    proj = Gather(lambda yy, xx, k: p_all.at[:, yy, xx, :, k], D)
    mixw = Gather(lambda yy, xx, k: m_all.at[:, yy, xx, :, k], 512)
    down = Gather(lambda yy, xx, k: d_all.at[:, yy, xx, :, k], 32 * FFB)

    local[1].wait()
    gate.a1()
    local[0].wait()
    own = xo.at[:, my_cols]
    row_tp = send(own, own, to_tp)
    row_up = send(xo.at[pl.ds(L - UP, UP), my_cols], xf.at[pl.ds(0, UP), my_cols], to_zr)
    row_low = send(xo.at[pl.ds(0, LOW), my_cols], xf.at[pl.ds(UP, LOW), my_cols], to_zl)
    local[2].wait()
    proj.a1()
    local[3].wait()
    mix_z = (
        send(wm.at[zo, :, pl.ds(0, 256)], m_all.at[zl, y, x, :, pl.ds(0, 256)], to_zr),
        send(wm.at[zo, :, pl.ds(256, 256)], m_all.at[zl, y, x, :, pl.ds(256, 256)], to_zl),
    )
    local[5].wait()
    kd = 16 * FFB
    u0, u1 = d_all.at[zl, y, x, :, pl.ds(0, kd)], d_all.at[zl, y, x, :, pl.ds(kd, kd)]
    down_z = (send(u0, u0, to_zr), send(u1, u1, to_zl))
    local[4].wait()

    def inverse_rms(src, dst, rows, step):
        def one(i, carry):
            at = pl.ds(pl.multiple_of(i * step, step), step)
            v = src[at, :].astype(F32)
            mean = jnp.sum(v * v, axis=-1, keepdims=True) * (1.0 / D)
            dst[at, :] = jnp.broadcast_to(lax.rsqrt(mean + EPS), (step, 128))
            return carry

        lax.fori_loop(0, rows // step, one, 0)

    row_tp.wait_recv()
    inverse_rms(xo, rs_o, L, 16)

    gate.a2()
    proj.a2()
    gate.a3()
    gate.z_own()
    for copy in mix_z:
        copy.wait_recv()
    mixw.a1()
    proj.a3()
    mixw.a2()
    row_up.wait_recv()
    u = xf.at[pl.ds(0, UP), my_cols]
    fwd_up = send(u, u, to_tp)
    row_low.wait_recv()
    u = xf.at[pl.ds(UP, LOW), my_cols]
    fwd_low = send(u, u, to_tp)
    gate.a4()
    gate.z_sides()
    mixw.a3()
    fwd_up.wait_recv()
    fwd_low.wait_recv()
    inverse_rms(xf, rs_f, FR, 16)
    up.a1()
    proj.a4()
    mixw.a4()
    gate.a5()
    gate.z_far()
    up.a2()
    for copy in down_z:
        copy.wait_recv()
    down.a1()
    up.a3()
    up.z_own()
    proj.a5()

    def mixer(rows_ref, rs, dst, groups):
        total = sum(groups)

        def tile(j, carry):
            def part(m):
                w = p_all[m, pl.ds(2 * j, 2)].reshape(256, D)
                return dot_t(rows_ref[...], w)

            r = rs[...]
            r = jnp.concatenate([r, r], axis=1)
            carried = (part(1) * r) * (part(2) * r)
            at = 0
            for g, n in enumerate(groups):
                c_s[pl.ds(at + 8 * g, 8), :] = jnp.zeros((8, 256), F32)
                c_s[pl.ds(at + 8 * g + 8, n), :] = carried[at:at + n]
                at += n
            outer = part(0) * r
            t_cols = pl.ds(pl.multiple_of(zl * 512 + j * 256, 256), 256)
            t0, t1, t2 = taps[0:1, t_cols], taps[1:2, t_cols], taps[2:3, t_cols]
            at = 0
            d_cols = pl.ds(pl.multiple_of(j * 256, 256), 256)
            for g, n in enumerate(groups):
                first = at + 8 * g + 8
                conv = (
                    t0 * c_s[pl.ds(first - 2, n), :]
                    + t1 * c_s[pl.ds(first - 1, n), :]
                    + t2 * c_s[pl.ds(first, n), :]
                )
                dst[pl.ds(at, n), d_cols] = (outer[at:at + n] * conv).astype(BF16)
                at += n
            return carry

        lax.fori_loop(0, 2, tile, 0)

    mixer(xf, rs_f, gf, (UP, LOW))
    up.a4()
    up.z_sides()
    down.a2()
    mixer(xo, rs_o, go, (L,))
    mixw.a5()
    down.a3()

    f_rows = pl.ds(HALO, L)
    cols = [pl.ds(j * 256, 256) for j in range(4)]

    def mtile(zz, j):
        return m_all[zz, j].reshape(256, 512)

    ex_f, ex_o = [], []
    for j in range(4):
        snd_f[:, cols[j]] = dot_t(gf[f_rows, :], mtile(1 - tp, j)).astype(BF16)
        ex_f.append(send(snd_f.at[:, cols[j]], rcv_f.at[:, cols[j]], to_tp))
    home = []
    for j in range(4):
        v = dot_t(gf[f_rows, :], mtile(tp, j))
        ex_f[j].wait_recv()
        fsum[:, cols[j]] = (v + rcv_f[:, cols[j]].astype(F32)).astype(BF16)
        a, b = pl.ds(0, LOW), pl.ds(LOW, LOW)
        home.append(send(fsum.at[a, cols[j]], rcv_z.at[b, cols[j]], to_zl))
        home.append(send(fsum.at[b, cols[j]], rcv_z.at[a, cols[j]], to_zr))
    up.a5()
    up.z_far()
    for j in range(4):
        snd_o[:, cols[j]] = dot_t(go[...], mtile(1 - tp, j)).astype(BF16)
        ex_o.append(send(snd_o.at[:, cols[j]], rcv_o.at[:, cols[j]], to_tp))
    for j in range(4):
        keep[:, cols[j]] = dot_t(go[...], mtile(tp, j))
    down.a4()
    ex_a = []
    for j in range(4):
        ex_o[j].wait_recv()
        home[2 * j].wait_recv()
        home[2 * j + 1].wait_recv()
        a_cols = pl.ds(pl.multiple_of(tp * HALF + j * 256, 256), 256)
        after = (
            xo[:, a_cols].astype(F32)
            + (keep[:, cols[j]] + rcv_o[:, cols[j]].astype(F32))
            + rcv_z[:, cols[j]].astype(F32)
        )
        af[:, a_cols] = after.astype(BF16)
        ex_a.append(send(af.at[:, a_cols], af.at[:, a_cols], to_tp))
    for copy in ex_a:
        copy.wait_recv()
    inverse_rms(af, rs_o, L, 16)

    gate.z_got()
    up.z_got()
    g_flat = g_all.reshape(2, 32 * FFB, D)

    def ffn_tile(t, carry):
        at = pl.ds(pl.multiple_of(t * 256, 256), 256)
        r = rs_o[...]
        r = jnp.concatenate([r, r], axis=1)
        g = dot_t(af[...], g_flat[0, at, :]) * r
        u = dot_t(af[...], g_flat[1, at, :]) * r
        hid[:, at] = (g / (1.0 + jnp.exp(-g)) * u).astype(BF16)
        return carry

    lax.fori_loop(0, 6, ffn_tile, 0)

    down.a5()

    def dtile(zz, j):
        return d_all[zz, j].reshape(256, 32 * FFB)

    ex_h = []
    for j in range(4):
        fsnd[:, cols[j]] = dot_t(hid[...], dtile(1 - tp, j)).astype(BF16)
        ex_h.append(send(fsnd.at[:, cols[j]], frcv.at[:, cols[j]], to_tp))
    back = []
    for j in range(4):
        v = dot_t(hid[...], dtile(tp, j))
        ex_h[j].wait_recv()
        a_cols = pl.ds(pl.multiple_of(tp * HALF + j * 256, 256), 256)
        total = af[:, a_cols].astype(F32) + (v + frcv[:, cols[j]].astype(F32))
        res[:, cols[j]] = total.astype(BF16)
        back.append(pltpu.make_async_copy(res.at[:, cols[j]], out.at[:, cols[j]], loc_sem.at[j]))
        back[-1].start()
    for copy in back:
        copy.wait()
    for copy in sent:
        copy.wait_send()


def body(
    sequence, mix_gain, ffn_gain, proj_outer, proj_inner, proj_value, proj_scales, taps,
    mix_out, mix_out_scale, ffn_gate, ffn_up, ffn_scales, ffn_down, down_scale,
):
    fs = lax.axis_index("fs")
    scales = lax.dynamic_slice(proj_scales, (0, fs * 32), (3, 32))
    wp = jnp.stack(
        [
            (w * mix_gain[:, None] * scales[i][None, :]).astype(BF16).T
            for i, w in enumerate((proj_outer, proj_inner, proj_value))
        ]
    )
    wm = (mix_out * mix_out_scale[None, :]).astype(BF16).T
    wm = jnp.moveaxis(wm.reshape(64, 2, 512), 1, 0)
    f_scales = lax.dynamic_slice(ffn_scales, (0, fs * 44), (2, 44))
    wg = jnp.stack(
        [
            (w * ffn_gain[:, None] * f_scales[i][None, :]).astype(BF16).T
            for i, w in enumerate((ffn_gate, ffn_up))
        ]
    )
    wg = jnp.pad(wg, ((0, 0), (0, FFB - 44), (0, 0)))
    wd = (ffn_down * down_scale[None, :]).astype(BF16).T
    wd = jnp.pad(wd.reshape(64, 32, 44), ((0, 0), (0, 0), (0, FFB - 44))).reshape(64, 32 * FFB)

    vm = pltpu.VMEM
    result = pl.pallas_call(
        kernel,
        out_shape=jax.ShapeDtypeStruct((L, HALF), BF16),
        in_specs=[pl.BlockSpec(memory_space=pl.ANY)] * 5 + [pl.BlockSpec(memory_space=vm)],
        out_specs=pl.BlockSpec(memory_space=pl.ANY),
        scratch_shapes=[
            vm((3, 4, 4, 32, D), BF16),
            vm((2, 4, 4, 64, 512), BF16),
            vm((2, 2, 4, 4, FFB, D), BF16),
            vm((2, 4, 4, 64, 32 * FFB), BF16),
            vm((L, D), BF16),
            vm((FR, D), BF16),
            vm((L, 512), BF16),
            vm((FR, 512), BF16),
            vm((FR + 16, 256), F32),
            vm((L, 128), F32),
            vm((FR, 128), F32),
            vm((L, HALF), BF16),
            vm((L, HALF), BF16),
            vm((L, HALF), BF16),
            vm((L, HALF), BF16),
            vm((L, HALF), F32),
            vm((L, HALF), BF16),
            vm((L, HALF), BF16),
            vm((L, D), BF16),
            vm((L, 32 * FFB), BF16),
            vm((L, HALF), BF16),
            vm((L, HALF), BF16),
            vm((L, HALF), BF16),
            pltpu.SemaphoreType.DMA((N_COPIES,)),
            pltpu.SemaphoreType.DMA((N_COPIES,)),
            pltpu.SemaphoreType.DMA((6,)),
        ],
        compiler_params=pltpu.CompilerParams(
            collective_id=0, has_side_effects=True, vmem_limit_bytes=67_000_000
        ),
        name="layer",
    )(sequence[0], wp, wm, wg, wd, taps)
    return result[None]


def solution(mesh):
    in_specs = (
        P(("rep", "fs"), None, "tp"),
        P(),
        P(),
        P(None, ("tp", "fs")),
        P(None, ("tp", "fs")),
        P(None, ("tp", "fs")),
        P(None, "tp"),
        P(None, "tp"),
        P("tp", "fs"),
        P("fs"),
        P(None, ("tp", "fs")),
        P(None, ("tp", "fs")),
        P(None, "tp"),
        P("tp", "fs"),
        P("fs"),
    )
    out_specs = P(("rep", "fs"), None, "tp")
    return jax.shard_map(body, mesh=mesh, in_specs=in_specs, out_specs=out_specs, check_vma=False)
```
